32 devices in a mesh: sp: 8 (over z, y), tp: 4 (over x, core).
Axes of the slice: x: 2, y: 2, z: 4, core: 2. Of those that a mesh axis runs over, the one named last changes fastest.
Arguments:
- resid: bfloat16 [8192, 2048], P(('sp', 'tp')), may hold values from -6 to 6
- query_nope: bfloat16 [8192, 2048], P('sp', 'tp'), may hold values from -18 to 18
- query_rope: bfloat16 [8192, 1024], P('sp', 'tp'), may hold values from -300 to 300
- latent: bfloat16 [8192, 256], P('sp'), may hold values from -6 to 6
- key_rope: bfloat16 [8192, 64], P('sp'), may hold values from -6 to 6
- latent_gain: float32 [256], replicated, may hold values from 0.1 to 1.9
- w_key: bfloat16 [256, 2048], P(None, 'tp'), may hold values from -0.375 to 0.375
- w_value: bfloat16 [256, 2048], P(None, 'tp'), may hold values from -0.375 to 0.375
- w_out: bfloat16 [2048, 2048], P('tp'), may hold values from -0.125 to 0.125
- mix_gain: float32 [2048], replicated, may hold values from 0.1 to 1.9
- w_gate: bfloat16 [2048, 5632], P('sp', 'tp'), may hold values from -0.125 to 0.125
- w_up: bfloat16 [2048, 5632], P('sp', 'tp'), may hold values from -0.125 to 0.125
- w_down: bfloat16 [2048, 5632], P('sp', 'tp'), may hold values from -0.078125 to 0.078125
Outputs:
- layer_out: bfloat16 [8192, 2048], P(('sp', 'tp'))
The draws below stay inside these ranges and needn't reach their ends.
All inputs are finite; a program needn't handle non-finite values.
Results may differ from the reference program's by a relative error of at most 0.0095.
Values may be sent and summed in bfloat16 or wider, within the bound.
A program may use at most 128 MiB of HBM per device.

```python
import jax
import jax.numpy as jnp
from jax import lax

D = 2048
HEADS = 16
NOPE = 128
ROPE = 64
VDIM = 128
RANK = 256
FF = 5632
TOK_DEV = 1024
TOKENS = 8192
N_SP = 8
N_TP = 4


def rope_pair(key):
    base_key = jax.random.fold_in(key, 11)
    key_one, key_two = jax.random.split(base_key, 2)
    key_part = jax.random.truncated_normal(key_one, -5.0, 5.0, (TOKENS, ROPE), jnp.float32)
    query_part = 3.0 * jax.random.truncated_normal(key_two, -5.0, 5.0, (TOKENS, HEADS * ROPE), jnp.float32)
    return (key_part, query_part)


def draw_query_rope(key, part):
    return rope_pair(key)[1].astype(jnp.bfloat16)


def draw_key_rope(key, part):
    return rope_pair(key)[0].astype(jnp.bfloat16)


def block_levels(key, dims, cuts, least, top_value):
    def one(position, blocks):
        heights = jax.random.uniform(jax.random.fold_in(jax.random.fold_in(key, 6), position), (blocks,), jnp.float32, least / len(cuts), top_value / len(cuts))
        return jnp.repeat(jnp.exp(heights), dims[position] // blocks).reshape((-1,) + (1,) * (len(dims) - position - 1))

    factor_of = one(*cuts[0])
    for cut in cuts[1:]:
        factor_of = factor_of * one(*cut)
    return factor_of


def bell_draw(stream_key, dims, spread, reach, cuts=(), held_as=jnp.bfloat16):
    loudness = block_levels(stream_key, dims, cuts, -0.22, 0.18) if cuts else 1.0
    result = jax.random.normal(stream_key, dims, jnp.float32) * spread * loudness
    return jnp.minimum(jnp.maximum(result, -reach), reach).astype(held_as)


def setup_inputs(seed: int = 0) -> dict:
    splits = jax.random.split(jax.random.key(seed), 14)
    resid = bell_draw(splits[0], (TOKENS, D), 1.0, 6.0, ((0, 32),))
    query_nope = bell_draw(splits[1], (TOKENS, HEADS * NOPE), 3.0, 18.0, ((0, 8), (1, 4)))
    query_rope = draw_query_rope(jax.random.fold_in(splits[13], 71), 0)
    latent = bell_draw(splits[3], (TOKENS, RANK), 1.0, 6.0, ((0, 8),))
    key_rope = draw_key_rope(jax.random.fold_in(splits[13], 71), 0)
    latent_gain = jnp.clip(1.0 + 0.18 * jax.random.normal(splits[5], (RANK,), jnp.float32), 0.1, 1.9)
    w_key = bell_draw(splits[6], (RANK, HEADS * NOPE), RANK ** -0.5, 0.375, ((1, 4),))
    w_value = bell_draw(splits[7], (RANK, HEADS * VDIM), RANK ** -0.5, 0.375, ((1, 4),))
    w_out = bell_draw(splits[8], (HEADS * VDIM, D), (HEADS * VDIM) ** -0.5, 0.125, ((0, 4),))
    mix_gain = jnp.clip(1.0 + 0.18 * jax.random.normal(splits[9], (D,), jnp.float32), 0.1, 1.9)
    w_gate = bell_draw(splits[10], (D, FF), D ** -0.5, 0.125, ((0, 8), (1, 4)))
    w_up = bell_draw(splits[11], (D, FF), D ** -0.5, 0.125, ((0, 8), (1, 4)))
    w_down = bell_draw(splits[12], (D, FF), FF ** -0.5, 0.078125, ((0, 8), (1, 4)))
    return {"resid": resid, "query_nope": query_nope, "query_rope": query_rope, "latent": latent, "key_rope": key_rope, "latent_gain": latent_gain, "w_key": w_key, "w_value": w_value, "w_out": w_out, "mix_gain": mix_gain, "w_gate": w_gate, "w_up": w_up, "w_down": w_down}


norm_eps = 1e-06
masked_score = -1e+30
theta_base = 10000.0

def rotate(values_in, angle):
    half_width = values_in.shape[-1] // 2
    front_half = values_in[..., :half_width]
    back_half = values_in[..., half_width:]
    cosine = jnp.cos(angle)
    sine_part = jnp.sin(angle)
    return jnp.concatenate([front_half * cosine - back_half * sine_part, back_half * cosine + front_half * sine_part], axis=-1)

def angles(positions, full_width):
    half_width = full_width // 2
    frequency = theta_base ** (-2.0 * jnp.arange(half_width).astype(jnp.float32) / full_width)
    return positions[:, None] * frequency[None, :]

def rms_scale(values_in, gain):
    return values_in * lax.rsqrt(lax.optimization_barrier(jnp.mean(values_in * values_in, axis=-1, keepdims=True)) + norm_eps) * gain

def reference(resid, query_nope, query_rope, latent, key_rope, latent_gain, w_key, w_value, w_out, mix_gain, w_gate, w_up, w_down):
    positions = jnp.arange(TOKENS).astype(jnp.float32)
    angle = angles(positions, ROPE)
    latent_normed = rms_scale(latent.astype(jnp.float32), latent_gain).astype(jnp.bfloat16)
    head_keys = jnp.dot(latent_normed, w_key, preferred_element_type=jnp.float32).astype(jnp.bfloat16)
    head_values = jnp.dot(latent_normed, w_value, preferred_element_type=jnp.float32).astype(jnp.bfloat16)
    key_rotated = rotate(key_rope.astype(jnp.float32), angle).astype(jnp.bfloat16)
    query_rotated = rotate(query_rope.astype(jnp.float32).reshape(TOKENS, HEADS, ROPE), angle[:, None, :]).astype(jnp.bfloat16)
    by_head_nope = jnp.transpose(query_nope.reshape(TOKENS, HEADS, NOPE), (1, 0, 2))
    by_head_rope = jnp.transpose(query_rotated, (1, 0, 2))
    by_head_keys = jnp.transpose(head_keys.reshape(TOKENS, HEADS, NOPE), (1, 0, 2))
    by_head_values = jnp.transpose(head_values.reshape(TOKENS, HEADS, VDIM), (1, 0, 2))
    score_scale = (NOPE + ROPE) ** (-0.5)
    key_positions = jnp.arange(TOKENS).astype(jnp.int32)

    def one_head(operands):
        nope_q, rope_q, keys_h, values_h = operands

        def one_block(block_index):
            first_row = block_index * TOK_DEV
            query_part = lax.dynamic_slice_in_dim(nope_q, first_row, TOK_DEV, 0)
            rope_part = lax.dynamic_slice_in_dim(rope_q, first_row, TOK_DEV, 0)
            scores = jnp.dot(query_part, keys_h.T, preferred_element_type=jnp.float32)
            scores = (scores + jnp.dot(rope_part, key_rotated.T, preferred_element_type=jnp.float32)) * score_scale
            query_rows = first_row + jnp.arange(TOK_DEV).astype(jnp.int32)
            causal = key_positions[None, :] <= query_rows[:, None]
            scores = jnp.where(causal, scores, masked_score)
            row_max = lax.optimization_barrier(jnp.max(scores, axis=-1, keepdims=True))
            weights = jnp.where(causal, jnp.exp(scores - row_max), 0.0)
            weight_sum = lax.optimization_barrier(jnp.sum(weights, axis=-1, keepdims=True))
            mixed = jnp.dot(weights.astype(jnp.bfloat16), values_h, preferred_element_type=jnp.float32)
            return (mixed / weight_sum).astype(jnp.bfloat16)
        return lax.map(one_block, jnp.arange(N_SP).astype(jnp.int32))
    head_out = lax.map(one_head, (by_head_nope, by_head_rope, by_head_keys, by_head_values))
    head_out = head_out.reshape(HEADS, TOKENS, VDIM)
    group_heads = HEADS // N_TP
    out_heads = w_out.reshape(HEADS, VDIM, D)
    attention_proj = jnp.zeros((TOKENS, D), jnp.float32)
    for group_index in range(N_TP):
        picked = slice(group_index * group_heads, (group_index + 1) * group_heads)
        partial_sum = jnp.einsum('htv,hvd->td', head_out[picked].astype(jnp.float32), out_heads[picked].astype(jnp.float32))
        attention_proj = attention_proj + lax.optimization_barrier(partial_sum.astype(jnp.bfloat16)).astype(jnp.float32)
    stream = resid.astype(jnp.float32) + attention_proj
    normed = rms_scale(stream, mix_gain).astype(jnp.bfloat16)
    group_units = FF // N_TP
    mixer_out = jnp.zeros((TOKENS, D), jnp.float32)
    for group_index in range(N_TP):
        columns = slice(group_index * group_units, (group_index + 1) * group_units)
        gate_value = jnp.dot(normed, w_gate[:, columns], preferred_element_type=jnp.float32)
        upward = jnp.dot(normed, w_up[:, columns], preferred_element_type=jnp.float32)
        hidden = (jax.nn.silu(gate_value) * upward).astype(jnp.bfloat16)
        partial_sum = jnp.dot(hidden, w_down[:, columns].T, preferred_element_type=jnp.float32)
        mixer_out = mixer_out + lax.optimization_barrier(partial_sum.astype(jnp.bfloat16)).astype(jnp.float32)
    return (stream + 0.5 * mixer_out).astype(jnp.bfloat16)
```

```python
import functools

import jax
import jax.numpy as jnp
from jax import lax
from jax.experimental import pallas as pl
from jax.experimental.pallas import tpu as pltpu
from jax.sharding import PartitionSpec as P

NOPE = 128
ROPE = 64
VDIM = 128
PAD = 64


norm_eps = 1e-06
masked_score = -1e30
theta_base = 10000.0
LOG2E = 1.4426950408889634
COLS = (((1,), (1,)), ((), ()))


def rotate(values_in, angle):
    half_width = values_in.shape[-1] // 2
    front_half = values_in[..., :half_width]
    back_half = values_in[..., half_width:]
    cosine = jnp.cos(angle)
    sine_part = jnp.sin(angle)
    return jnp.concatenate(
        [front_half * cosine - back_half * sine_part, back_half * cosine + front_half * sine_part],
        axis=-1,
    )


def angles(positions, full_width):
    half_width = full_width // 2
    frequency = theta_base ** (-2.0 * jnp.arange(half_width).astype(jnp.float32) / full_width)
    return positions[:, None] * frequency[None, :]


def rms_scale(values_in, gain):
    return (
        values_in
        * lax.rsqrt(jnp.mean(values_in * values_in, axis=-1, keepdims=True) + norm_eps)
        * gain
    )


def attention_kernel(tile, q_ref, lat_ref, wk_ref, wv_ref, o_ref, k_ref, v_ref, m_ref, acc_ref):
    step = pl.program_id(0)
    me = lax.axis_index("sp")
    heads, rows, width = q_ref.shape
    rank = wk_ref.shape[1]
    tiles = rows // tile
    scale = (NOPE + ROPE) ** (-0.5) * LOG2E

    @pl.when(step == 0)
    def _():
        m_ref[...] = jnp.full_like(m_ref, masked_score)
        acc_ref[...] = jnp.zeros_like(acc_ref)

    def project(h):
        block = lat_ref[:, :rank]
        keys = jnp.dot(block, wk_ref[h], preferred_element_type=jnp.float32)
        k_ref[:, :NOPE] = keys.astype(jnp.bfloat16)
        k_ref[:, NOPE:] = lat_ref[:, rank:]
        values = jnp.dot(block, wv_ref[h], preferred_element_type=jnp.float32)
        v_ref[:, :VDIM] = values.astype(jnp.bfloat16)
        v_ref[:, VDIM:] = jnp.ones((rows, width - VDIM), jnp.bfloat16)

    def fold(h, t, keys, diagonal):
        span = pl.ds(t * tile, tile)
        scores = lax.dot_general(
            q_ref[h, span, :], k_ref[:keys, :], COLS, preferred_element_type=jnp.float32
        )
        if diagonal:
            row = t * tile + lax.broadcasted_iota(jnp.int32, scores.shape, 0)
            col = lax.broadcasted_iota(jnp.int32, scores.shape, 1)
            scores = jnp.where(col <= row, scores, masked_score)
        old = m_ref[h, span, :]
        top = jnp.maximum(old, jnp.max(scores, axis=1, keepdims=True))
        weights = jnp.exp2((scores - top[:, :1]) * scale)
        factor = jnp.exp2((old - top) * scale)
        mixed = jnp.dot(
            weights.astype(jnp.bfloat16), v_ref[:keys, :], preferred_element_type=jnp.float32
        )
        m_ref[h, span, :] = top
        acc_ref[h, span, :] = acc_ref[h, span, :] * factor[:, :1] + mixed

    @pl.when(step < me)
    def _():
        def one_head(h, carry):
            project(h)
            for t in range(tiles):
                fold(h, t, rows, False)
            return carry

        lax.fori_loop(0, heads, one_head, 0)

    @pl.when(step == me)
    def _():
        def one_head(h, carry):
            project(h)
            for t in range(tiles):
                fold(h, t, (t + 1) * tile, True)
            done = acc_ref[h]
            out = done[:, :VDIM] / done[:, VDIM : 2 * VDIM]
            o_ref[h] = out.astype(o_ref.dtype)
            return carry

        lax.fori_loop(0, heads, one_head, 0)


def attention(q, lat, wk, wv, steps):
    heads, rows, width = q.shape
    tile = next(size for size in (256, 128, 64, 32, 16, 8) if rows % size == 0)
    whole = lambda shape: pl.BlockSpec(shape, lambda j: (0,) * len(shape))
    flops = 2 * rows * rows * steps * heads * (width + width)
    return pl.pallas_call(
        functools.partial(attention_kernel, tile),
        grid=(steps,),
        out_shape=jax.ShapeDtypeStruct((heads, rows, VDIM), jnp.bfloat16),
        in_specs=[
            whole(q.shape),
            pl.BlockSpec((rows, lat.shape[1]), lambda j: (j, 0)),
            whole(wk.shape),
            whole(wv.shape),
        ],
        out_specs=whole((heads, rows, VDIM)),
        scratch_shapes=[
            pltpu.VMEM((rows, width), jnp.bfloat16),
            pltpu.VMEM((rows, width), jnp.bfloat16),
            pltpu.VMEM((heads, rows, 128), jnp.float32),
            pltpu.VMEM((heads, rows, width), jnp.float32),
        ],
        compiler_params=pltpu.CompilerParams(
            dimension_semantics=("arbitrary",), vmem_limit_bytes=48 * 1024 * 1024
        ),
        cost_estimate=pl.CostEstimate(
            flops=flops, bytes_accessed=2 * rows * 512 * steps, transcendentals=rows * rows * steps
        ),
    )(q, lat, wk, wv)


def on_device(
    n_sp,
    resid,
    query_nope,
    query_rope,
    latent,
    key_rope,
    latent_gain,
    w_key,
    w_value,
    w_out,
    mix_gain,
    w_gate,
    w_up,
    w_down,
):
    row_count = query_nope.shape[0]
    head_count = query_nope.shape[1] // NOPE
    rank = latent.shape[1]
    first_row = lax.axis_index("sp") * row_count
    query_rows = first_row + jnp.arange(row_count, dtype=jnp.int32)
    angle = angles(query_rows.astype(jnp.float32), ROPE)
    latent_normed = rms_scale(latent.astype(jnp.float32), latent_gain).astype(jnp.bfloat16)
    key_rotated = rotate(key_rope.astype(jnp.float32), angle).astype(jnp.bfloat16)
    packed = jnp.concatenate(
        [latent_normed, key_rotated, jnp.zeros((row_count, PAD), jnp.bfloat16)], axis=-1
    )
    latent_all = lax.all_gather(packed, "sp", axis=0, tiled=True)
    gate_full, up_full, down_full = (
        lax.all_gather(w_gate, "sp", axis=0, tiled=True),
        lax.all_gather(w_up, "sp", axis=0, tiled=True),
        lax.all_gather(w_down, "sp", axis=0, tiled=True),
    )
    rope_query = rotate(
        query_rope.astype(jnp.float32).reshape(row_count, head_count, ROPE), angle[:, None, :]
    ).astype(jnp.bfloat16)
    queries = jnp.concatenate(
        [
            query_nope.reshape(row_count, head_count, NOPE),
            rope_query,
            jnp.zeros((row_count, head_count, PAD), jnp.bfloat16),
        ],
        axis=-1,
    ).transpose(1, 0, 2)
    wk = w_key.reshape(rank, head_count, NOPE).transpose(1, 0, 2)
    wv = w_value.reshape(rank, head_count, VDIM).transpose(1, 0, 2)
    head_out = attention(queries, latent_all, wk, wv, n_sp)
    out_heads = w_out.reshape(head_count, VDIM, w_out.shape[1])
    head_term = jnp.einsum("hqv,hvd->qd", head_out, out_heads, preferred_element_type=jnp.float32)
    attention_proj = lax.psum_scatter(
        head_term.astype(jnp.bfloat16), "tp", scatter_dimension=0, tiled=True
    ).astype(jnp.float32)
    stream = resid.astype(jnp.float32) + attention_proj
    normed = rms_scale(stream, mix_gain).astype(jnp.bfloat16)
    row_piece = lax.all_gather(normed, "tp", axis=0, tiled=True)
    gate_value = jnp.dot(row_piece, gate_full, preferred_element_type=jnp.float32)
    upward = jnp.dot(row_piece, up_full, preferred_element_type=jnp.float32)
    hidden = (jax.nn.silu(gate_value) * upward).astype(jnp.bfloat16)
    down_term = lax.dot_general(hidden, down_full, COLS, preferred_element_type=jnp.float32)
    mixer_out = lax.psum_scatter(
        down_term.astype(jnp.bfloat16), "tp", scatter_dimension=0, tiled=True
    ).astype(jnp.float32)
    return (stream + 0.5 * mixer_out).astype(jnp.bfloat16)


def solution(mesh):
    return jax.shard_map(
        functools.partial(on_device, mesh.shape["sp"]),
        mesh=mesh,
        in_specs=(
            P(("sp", "tp"), None),
            P("sp", "tp"),
            P("sp", "tp"),
            P("sp", None),
            P("sp", None),
            P(),
            P(None, "tp"),
            P(None, "tp"),
            P("tp", None),
            P(),
            P("sp", "tp"),
            P("sp", "tp"),
            P("sp", "tp"),
        ),
        out_specs=P(("sp", "tp"), None),
        check_vma=False,
    )
```

```python
import functools

import jax
import jax.numpy as jnp
from jax import lax
from jax.experimental import pallas as pl
from jax.experimental.pallas import tpu as pltpu
from jax.sharding import PartitionSpec as P

NOPE = 128
ROPE = 64
VDIM = 128
PAD = 64


norm_eps = 1e-06
masked_score = -1e30
theta_base = 10000.0
LOG2E = 1.4426950408889634
COLS = (((1,), (1,)), ((), ()))


def rotate(values_in, angle):
    half_width = values_in.shape[-1] // 2
    front_half = values_in[..., :half_width]
    back_half = values_in[..., half_width:]
    cosine = jnp.cos(angle)
    sine_part = jnp.sin(angle)
    return jnp.concatenate(
        [front_half * cosine - back_half * sine_part, back_half * cosine + front_half * sine_part],
        axis=-1,
    )


def angles(positions, full_width):
    half_width = full_width // 2
    frequency = theta_base ** (-2.0 * jnp.arange(half_width).astype(jnp.float32) / full_width)
    return positions[:, None] * frequency[None, :]


def rms_scale(values_in, gain):
    return (
        values_in
        * lax.rsqrt(jnp.mean(values_in * values_in, axis=-1, keepdims=True) + norm_eps)
        * gain
    )


def ring_order(count):
    narrow = 1
    while (2 * narrow) ** 2 <= count and count % (2 * narrow) == 0:
        narrow *= 2
    long = count // narrow
    if narrow == 1 or long % 2:
        return list(range(count))
    order = []
    for row in range(long):
        columns = range(1, narrow) if row % 2 == 0 else range(narrow - 1, 0, -1)
        order += [row * narrow + column for column in columns]
    return order + [row * narrow for row in reversed(range(long))]


def attention_kernel(tile, q_ref, lat_ref, wk_ref, wv_ref, o_ref, k_ref, v_ref, m_ref, acc_ref):
    step = pl.program_id(0)
    me = lax.axis_index("sp")
    heads, rows, width = q_ref.shape
    rank = wk_ref.shape[1]
    tiles = rows // tile
    group = 2 if tiles % 2 == 0 else 1
    scale = (NOPE + ROPE) ** (-0.5) * LOG2E

    @pl.when(step == 0)
    def _():
        m_ref[...] = jnp.full_like(m_ref, masked_score)
        acc_ref[...] = jnp.zeros_like(acc_ref)

    def project(h):
        block = lat_ref[:, :rank]
        keys = jnp.dot(block, wk_ref[h], preferred_element_type=jnp.float32)
        k_ref[:, :NOPE] = keys.astype(jnp.bfloat16)
        k_ref[:, NOPE:] = lat_ref[:, rank:]
        values = jnp.dot(block, wv_ref[h], preferred_element_type=jnp.float32)
        v_ref[:, :VDIM] = values.astype(jnp.bfloat16)
        v_ref[:, VDIM:] = jnp.ones((rows, width - VDIM), jnp.bfloat16)

    def fold(h, t, keys, diagonal):
        span = pl.ds(pl.multiple_of(t * tile, tile), tile)
        scores = lax.dot_general(
            q_ref[h, span, :], k_ref[:keys, :], COLS, preferred_element_type=jnp.float32
        )
        if diagonal:
            row = t * tile + lax.broadcasted_iota(jnp.int32, scores.shape, 0)
            col = lax.broadcasted_iota(jnp.int32, scores.shape, 1)
            scores = jnp.where(col <= row, scores, masked_score)
        old = m_ref[h, span, :]
        top = jnp.maximum(old, jnp.max(scores, axis=1, keepdims=True))
        weights = jnp.exp2((scores - top[:, :1]) * scale)
        factor = jnp.exp2((old - top) * scale)
        mixed = jnp.dot(
            weights.astype(jnp.bfloat16), v_ref[:keys, :], preferred_element_type=jnp.float32
        )
        m_ref[h, span, :] = top
        acc_ref[h, span, :] = acc_ref[h, span, :] * factor[:, :1] + mixed

    @pl.when(step < me)
    def _():
        def one_head(h, carry):
            project(h)
            def some_tiles(i, inner):
                for t in range(group):
                    fold(h, i * group + t, rows, False)
                return inner

            return lax.fori_loop(0, tiles // group, some_tiles, carry)

        lax.fori_loop(0, heads, one_head, 0)

    @pl.when(step == me)
    def _():
        def one_head(h, carry):
            project(h)
            for t in range(tiles):
                fold(h, t, (t + 1) * tile, True)
            done = acc_ref[h]
            out = done[:, :VDIM] / done[:, VDIM : 2 * VDIM]
            o_ref[h] = out.astype(o_ref.dtype)
            return carry

        lax.fori_loop(0, heads, one_head, 0)


def attention(q, lat, wk, wv, steps):
    heads, rows, width = q.shape
    tile = next(size for size in (256, 128, 64, 32, 16, 8) if rows % size == 0)
    whole = lambda shape: pl.BlockSpec(shape, lambda j: (0,) * len(shape))
    flops = 4 * rows * rows * steps * heads * (width + width)
    return pl.pallas_call(
        functools.partial(attention_kernel, tile),
        grid=(steps,),
        out_shape=jax.ShapeDtypeStruct((heads, rows, VDIM), jnp.bfloat16),
        in_specs=[
            whole(q.shape),
            pl.BlockSpec((rows, lat.shape[1]), lambda j: (j, 0)),
            whole(wk.shape),
            whole(wv.shape),
        ],
        out_specs=whole((heads, rows, VDIM)),
        scratch_shapes=[
            pltpu.VMEM((rows, width), jnp.bfloat16),
            pltpu.VMEM((rows, width), jnp.bfloat16),
            pltpu.VMEM((heads, rows, 128), jnp.float32),
            pltpu.VMEM((heads, rows, width), jnp.float32),
        ],
        compiler_params=pltpu.CompilerParams(
            dimension_semantics=("arbitrary",), vmem_limit_bytes=48 * 1024 * 1024
        ),
        cost_estimate=pl.CostEstimate(
            flops=flops, bytes_accessed=2 * rows * 512 * steps, transcendentals=rows * rows * steps
        ),
    )(q, lat, wk, wv)


def on_device(
    n_sp,
    n_tp,
    resid,
    query_nope,
    query_rope,
    latent,
    key_rope,
    latent_gain,
    w_key,
    w_value,
    w_out,
    mix_gain,
    w_gate,
    w_up,
    w_down,
):
    row_count = query_nope.shape[0]
    head_count = query_nope.shape[1] // NOPE
    rank = latent.shape[1]
    first_row = lax.axis_index("sp") * row_count
    query_rows = first_row + jnp.arange(row_count, dtype=jnp.int32)
    angle = angles(query_rows.astype(jnp.float32), ROPE)
    latent_normed = rms_scale(latent.astype(jnp.float32), latent_gain).astype(jnp.bfloat16)
    key_rotated = rotate(key_rope.astype(jnp.float32), angle).astype(jnp.bfloat16)
    packed = jnp.concatenate(
        [latent_normed, key_rotated, jnp.zeros((row_count, PAD), jnp.bfloat16)], axis=-1
    )
    share = row_count // n_tp
    packed = lax.dynamic_slice_in_dim(packed, lax.axis_index("tp") * share, share, 0)
    latent_all = lax.all_gather(packed, ("sp", "tp"), axis=0, tiled=True)
    order = ring_order(n_sp)
    weights = jnp.stack([w_gate, w_up, w_down])
    part = weights.shape[1]
    half = part // 2
    travelling = [weights[:, :half], weights[:, half:]]
    place = jnp.array([order.index(i) for i in range(n_sp)], jnp.int32)[lax.axis_index("sp")]
    table = jnp.array(order, jnp.int32)
    ahead = [(order[i], order[(i + 1) % n_sp]) for i in range(n_sp)]
    back = [(dst, src) for src, dst in ahead]
    full = jnp.zeros((weights.shape[0], part * n_sp, weights.shape[2]), jnp.bfloat16)
    full = lax.dynamic_update_slice(full, weights, (0, lax.axis_index("sp") * part, 0))

    def hop(number, full, travelling):
        moved = [
            lax.ppermute(travelling[0], "sp", ahead),
            lax.ppermute(travelling[1], "sp", back),
        ]
        for piece, owner, offset in (
            (moved[0], table[(place - number) % n_sp], 0),
            (moved[1], table[(place + number) % n_sp], half),
        ):
            full = lax.dynamic_update_slice(full, piece, (0, owner * part + offset, 0))
        return full, moved

    rope_query = rotate(
        query_rope.astype(jnp.float32).reshape(row_count, head_count, ROPE), angle[:, None, :]
    ).astype(jnp.bfloat16)
    queries = jnp.concatenate(
        [
            query_nope.reshape(row_count, head_count, NOPE),
            rope_query,
            jnp.zeros((row_count, head_count, PAD), jnp.bfloat16),
        ],
        axis=-1,
    ).transpose(1, 0, 2)
    wk = w_key.reshape(rank, head_count, NOPE).transpose(1, 0, 2)
    wv = w_value.reshape(rank, head_count, VDIM).transpose(1, 0, 2)
    heads_out = []
    hops_done = 0

    def advance(value, full, travelling, hops_done):
        if hops_done < n_sp - 1:
            full, travelling = hop(hops_done + 1, full, travelling)
            value, *travelling = lax.optimization_barrier((value, *travelling))
            hops_done += 1
        return value, full, travelling, hops_done

    for h in range(head_count):
        query, full, travelling, hops_done = advance(
            queries[h : h + 1], full, travelling, hops_done
        )
        if h == 0:
            latent_all, *travelling = lax.optimization_barrier((latent_all, *travelling))
        heads_out.append(attention(query, latent_all, wk[h : h + 1], wv[h : h + 1], n_sp))
        if h and hops_done < n_sp - 1:
            heads_out[h - 1], *travelling = lax.optimization_barrier(
                (heads_out[h - 1], *travelling)
            )
    head_out = jnp.concatenate(heads_out)
    out_heads = w_out.reshape(head_count, VDIM, w_out.shape[1])
    head_term = jnp.einsum("hqv,hvd->qd", head_out, out_heads, preferred_element_type=jnp.float32)
    head_term, full, travelling, hops_done = advance(
        head_term.astype(jnp.bfloat16), full, travelling, hops_done
    )
    attention_proj = lax.psum_scatter(head_term, "tp", scatter_dimension=0, tiled=True).astype(
        jnp.float32
    )
    stream = resid.astype(jnp.float32) + attention_proj
    normed = rms_scale(stream, mix_gain).astype(jnp.bfloat16)
    normed, full, travelling, hops_done = advance(normed, full, travelling, hops_done)
    while hops_done < n_sp - 1:
        full, travelling = hop(hops_done + 1, full, travelling)
        hops_done += 1
    gate_full, up_full, down_full = full[0], full[1], full[2]
    row_piece = lax.all_gather(normed, "tp", axis=0, tiled=True)
    gate_value = jnp.dot(row_piece, gate_full, preferred_element_type=jnp.float32)
    upward = jnp.dot(row_piece, up_full, preferred_element_type=jnp.float32)
    hidden = (jax.nn.silu(gate_value) * upward).astype(jnp.bfloat16)
    down_term = lax.dot_general(hidden, down_full, COLS, preferred_element_type=jnp.float32)
    mixer_out = lax.psum_scatter(
        down_term.astype(jnp.bfloat16), "tp", scatter_dimension=0, tiled=True
    ).astype(jnp.float32)
    return (stream + 0.5 * mixer_out).astype(jnp.bfloat16)


def solution(mesh):
    return jax.shard_map(
        functools.partial(on_device, mesh.shape["sp"], mesh.shape["tp"]),
        mesh=mesh,
        in_specs=(
            P(("sp", "tp"), None),
            P("sp", "tp"),
            P("sp", "tp"),
            P("sp", None),
            P("sp", None),
            P(),
            P(None, "tp"),
            P(None, "tp"),
            P("tp", None),
            P(),
            P("sp", "tp"),
            P("sp", "tp"),
            P("sp", "tp"),
        ),
        out_specs=P(("sp", "tp"), None),
        check_vma=False,
    )
```
